512 devices in a mesh: row: 32 (over z, x), col: 16 (over y, core).
Axes of the slice: x: 4, y: 8, z: 8, core: 2. Of those that a mesh axis runs over, the one named last changes fastest.
Arguments:
- tokens: bfloat16 [32768, 2048], P('row'), may hold values from -136 to 136
- norm_gain: float32 [2048], replicated, may hold values from 0.1 to 1.9
- w_in: bfloat16 [2048, 1024], P(None, 'col'), may hold values from -0.125 to 0.125
- w_out: bfloat16 [1024, 2048], P(None, 'col'), may hold values from -0.1875 to 0.1875
Outputs:
- mixed_tokens: bfloat16 [32768, 2048], P('row', 'col')
The draws below stay inside these ranges and needn't reach their ends.
All inputs are finite; a program needn't handle non-finite values.
Results may differ from the reference program's by a relative error of at most 0.013.
Values may be sent and summed in bfloat16 or wider, within the bound.
A program may use at most 64 MiB of HBM per device.

```python
import math
import jax
import jax.numpy as jnp
from jax import lax

D = 2048
FW = 1024
GROUP = 256
GROUPS = 4
LENGTH = 32768


def draw_tokens(key, part):
    key_values, key_scales = jax.random.split(key, 2)
    columns = jnp.arange(D, dtype=jnp.float32) / D
    values = jnp.clip(jax.random.normal(key_values, (LENGTH, D), jnp.float32), -6.0, 6.0)
    row_scale = jnp.exp(jax.random.uniform(key_scales, (LENGTH, 1), jnp.float32, 0.0, 0.2))
    col_scale = jnp.exp(columns * math.log(4.0))
    return (values * row_scale * col_scale[None, :]).astype(jnp.bfloat16)


def level_of(own_key, extent, cuts, smallest, high):
    factor_of, own = 1.0, jax.random.fold_in(own_key, 6)
    for position, shards_of in cuts:
        steps = jnp.exp(jax.random.uniform(jax.random.fold_in(own, position), (shards_of,), jnp.float32, smallest / len(cuts), high / len(cuts)))
        factor_of = factor_of * jnp.repeat(steps, extent[position] // shards_of).reshape([-1 if axis == position else 1 for axis in range(len(extent))])
    return factor_of


def bell_draw(rng, dims, spread, most, cuts=(), kind=jnp.bfloat16):
    drawn = jax.random.normal(rng, dims, jnp.float32) * spread
    if len(cuts) > 0:
        drawn = level_of(rng, dims, cuts, -0.22, 0.18) * drawn
    return jnp.clip(drawn, min=-most, max=most).astype(kind)


def setup_inputs(seed: int = 0) -> dict:
    keys = jax.random.split(jax.random.key(seed), 5)
    tokens = draw_tokens(jax.random.fold_in(keys[4], 71), 0)
    norm_gain = jnp.clip(1.0 + 0.18 * jax.random.normal(keys[1], (D,), jnp.float32), 0.1, 1.9)
    w_in = bell_draw(keys[2], (D, FW), D ** -0.5, 0.125, ((1, 16),))
    w_out = bell_draw(keys[3], (FW, D), FW ** -0.5, 0.1875, ((1, 16),))
    return {"tokens": tokens, "norm_gain": norm_gain, "w_in": w_in, "w_out": w_out}


NORM_EPS = 1e-06

def reference(tokens, norm_gain, w_in, w_out):
    widened = tokens.astype(jnp.float32)
    inverse = lax.rsqrt(lax.optimization_barrier(jnp.mean(widened * widened, axis=1, keepdims=True)) + NORM_EPS)
    normed = (widened * inverse * norm_gain[None, :]).astype(jnp.bfloat16)
    projected = jnp.dot(normed, w_in, preferred_element_type=jnp.float32).astype(jnp.bfloat16)
    grouped = projected.astype(jnp.float32).reshape(LENGTH, GROUPS, GROUP)
    spectrum = jnp.real(jnp.fft.fftn(grouped, axes=(0, 2), norm='ortho'))
    spectral = spectrum.reshape(LENGTH, FW).astype(jnp.bfloat16)
    return jnp.dot(spectral, w_out, preferred_element_type=jnp.float32).astype(jnp.bfloat16)
```

```python
import functools
import math

import jax
import jax.numpy as jnp
import ml_dtypes
import numpy as np
from jax import lax
from jax.experimental import pallas as pl
from jax.experimental.pallas import tpu as pltpu
from jax.sharding import PartitionSpec as P

GROUP = 256
NORM_EPS = 1e-06
LANES = 128
PIECES = 4
MESH = pl.DeviceIdType.MESH
BF16 = jnp.bfloat16
F32 = jnp.float32


def angle(first, second, period):
    return (np.multiply.outer(first, second) % period) * (2.0 * math.pi / period)


def tables(rows, width, length):
    subs = GROUP // width
    pairs = np.arange(GROUP // 2)
    channel = np.arange(GROUP)
    cosine, sine = np.cos(angle(pairs, channel, GROUP)), np.sin(angle(pairs, channel, GROUP))
    sine[0] = np.cos(math.pi * channel)
    mix = np.stack([cosine, sine], 1).reshape(GROUP, GROUP) / math.sqrt(GROUP)

    back = np.zeros((subs, 2, rows, GROUP))
    for p in range(GROUP // 2):
        j, r = divmod(p, rows)
        if p == 0:
            back[j, 0, r, 0] = 1.0
            back[j, 1, r, GROUP // 2] = 1.0
        else:
            back[j, 0, r, p] = back[j, 0, r, GROUP - p] = 1.0
            back[j, 1, r, GROUP - p] = 1.0
            back[j, 1, r, p] = -1.0
    back = back.reshape(GROUP, GROUP)

    total = rows * length
    high = total // LANES
    steps = length // LANES
    a = np.arange(high)
    turn = angle(a, a, high)
    outer = np.zeros((2, 2, high, rows, 2, steps))
    for s in range(2):
        outer[s, 0, :, :, s, :] = np.cos(turn).reshape(high, rows, steps)
        outer[s, 1, :, :, s, :] = -np.sin(turn).reshape(high, rows, steps)
    outer = outer.reshape(4 * high, 2 * high) / math.sqrt(high)

    b = np.arange(LANES)
    twist = angle(a, b, total)
    twist = np.concatenate([np.cos(twist), np.sin(twist)], 0)

    turn = angle(b, b, LANES)
    cosine, sine = np.cos(turn), np.sin(turn)
    inner = np.stack([np.concatenate([cosine, sine], 1), np.concatenate([sine, -cosine], 1)]) / math.sqrt(LANES)
    short = ml_dtypes.bfloat16
    return mix.astype(short), back.astype(short), outer.astype(short), twist.astype(np.float32), inner.astype(short), np.eye(width).astype(short)


def nt(a, b):
    return lax.dot_general(a, b, (((1,), (1,)), ((), ())), preferred_element_type=F32)


def nn(a, b):
    return jnp.dot(a, b, preferred_element_type=F32)


def kernel(
    rows, cols,
    tokens, gain, w_in, w_out, mix, back, outer, twist, inner, eye, out,
    tok_v, tg_v, sq_v, gain_v, win_v, wout_v, mix_v, back_v, outer_v, twist_v, inner_v, eye_v,
    x_v, wide_v, a_v, ar_v, b_v, br_v, s_v, wt_v, acc_v,
    tok_sem, tab_sem, xs_sem, xr_sem, as_sem, ar_sem, bs_sem, br_sem, gs_sem, gr_sem, cs_sem, cr_sem,
):
    length, features = tokens.shape
    width = w_in.shape[1]
    subs = GROUP // width
    piece = length // PIECES
    steps = length // LANES
    tile = 2 * steps
    row, col = lax.axis_index("row"), lax.axis_index("col")
    core = lax.rem(col, 2)
    other = col + 1 - 2 * core
    chip = lax.div(col, 2)
    twin = col + 2 - 4 * lax.rem(chip, 2)
    right, left = lax.rem(col + 2, cols), lax.rem(col + cols - 2, cols)
    j = lax.rem(col, subs)

    def load(src, dst, sem):
        return pltpu.make_async_copy(src, dst, sem)

    def send(src, dst, send_sem, recv_sem, device):
        return pltpu.make_async_remote_copy(
            src_ref=src, dst_ref=dst, send_sem=send_sem, recv_sem=recv_sem, device_id=device, device_id_type=MESH
        )

    loads = [load(gain, gain_v, tab_sem.at[0]), load(w_in, win_v, tab_sem.at[1]), load(eye, eye_v, tab_sem.at[2])]
    for c in loads:
        c.start()
    tok = [
        load(tokens.at[pl.ds(p * piece, piece)], tok_v.at[pl.ds(p * piece, piece)], tok_sem.at[p]) for p in range(PIECES)
    ]
    for c in tok:
        c.start()
    later = [
        load(src, dst, tab_sem.at[3 + i])
        for i, (src, dst) in enumerate(
            ((mix, mix_v), (outer, outer_v), (w_out, wout_v), (back, back_v), (twist, twist_v), (inner, inner_v))
        )
    ]
    for c in later:
        c.start()

    barrier = pltpu.get_barrier_semaphore()
    for mate in (other, right, left):
        pl.semaphore_signal(barrier, inc=1, device_id=(row, mate), device_id_type=MESH)

    def greet(i, carry):
        pl.semaphore_signal(barrier, inc=1, device_id=(lax.rem(row + i, rows), col), device_id_type=MESH)
        return carry

    lax.fori_loop(1, rows, greet, 0)

    for c in loads:
        c.wait()

    def x_slot(p, who):
        return x_v.at[p, pl.ds(pl.multiple_of(lax.rem(who, subs) * width, width), width)]

    to_other = [send(x_slot(p, col), x_slot(p, col), xs_sem.at[0, p], xr_sem.at[0, p], (row, other)) for p in range(PIECES)]
    to_twin = [send(x_slot(p, col), x_slot(p, col), xs_sem.at[1, p], xr_sem.at[1, p], (row, twin)) for p in range(PIECES)]
    onward = [send(x_slot(p, twin), x_slot(p, twin), xs_sem.at[2, p], xr_sem.at[2, p], (row, other)) for p in range(PIECES)]
    block = 64
    for p in range(PIECES):
        tok[p].wait()

        def scaled(i, carry):
            at = pl.multiple_of(i * block, block)
            t = tok_v[pl.ds(p * piece + at, block), :].astype(F32)
            sq_v[pl.ds(at, block), :] = jnp.broadcast_to(jnp.sum(t * t, axis=1, keepdims=True), (block, LANES))
            tg_v[pl.ds(at, block), :] = (t * gain_v[...]).astype(BF16)
            return carry

        lax.fori_loop(0, piece // block, scaled, 0)
        x = nn(tg_v[...], win_v[...])
        x = x * lax.rsqrt(sq_v[:, :width] * (1.0 / features) + NORM_EPS)
        x_v[p, pl.ds(pl.multiple_of(j * width, width), width), :] = nt(eye_v[...], x.astype(BF16)).astype(BF16)
        if p == 0:
            pl.semaphore_wait(barrier, rows + 2)
        to_twin[p].start()
        to_other[p].start()
    for p in range(PIECES):
        to_twin[p].wait_recv()
        onward[p].start()

    for c in later:
        c.wait()
    mine = mix_v[pl.ds(pl.multiple_of(j * width, width), width), :]
    for p in range(PIECES):
        to_other[p].wait_recv()
        onward[p].wait_recv()
        y = nn(mine, x_v[p])
        for t in range(piece // LANES):
            wide_v[pl.ds(p * (piece // LANES) + t, width, stride=steps), :] = y[:, t * LANES : (t + 1) * LANES]
    a_v[...] = wide_v[...].astype(BF16)

    def spread(src_v, dst_v, send_sem, recv_sem):
        own = pl.ds(pl.multiple_of(row * tile, tile), tile)

        def one(i, carry):
            d = lax.rem(row + i, rows)
            send(
                src_v.at[pl.ds(pl.multiple_of(d * tile, tile), tile)], dst_v.at[own], send_sem, recv_sem, (d, col)
            ).start()
            return carry

        lax.fori_loop(1, rows, one, 0)
        dst_v[own, :] = src_v[own, :]

    rest = pl.ds(0, (rows - 1) * tile)
    spread(a_v, ar_v, as_sem, ar_sem)

    per_group = 2 * LANES // GROUP if GROUP < 2 * LANES else GROUP // (2 * width)
    for g in range(cols // subs):
        wp = nn(back_v[...], wout_v[pl.ds(g * GROUP, GROUP), :])
        for i in range(per_group):
            wt_v[g * per_group + i] = jnp.transpose(wp[i * 2 * width : (i + 1) * 2 * width]).astype(BF16)

    load(ar_v.at[rest], ar_v.at[rest], ar_sem).wait()

    first = nn(outer_v[...], ar_v[...])
    high = rows * steps
    twist_cos, twist_sin = twist_v[:high], twist_v[high:]
    special = lax.min(j * rows + row, 1)
    for s in range(2):
        re = first[2 * s * high : (2 * s + 1) * high]
        im = first[(2 * s + 1) * high : (2 * s + 2) * high]
        turned = jnp.concatenate([re * twist_cos + im * twist_sin, im * twist_cos - re * twist_sin], axis=1).astype(BF16)
        u = nt(inner_v[0] if s == 0 else inner_v[special], turned)
        for t in range(2):
            wide_v[pl.ds(2 * t + s, LANES, stride=4), :] = u[:, t * LANES : (t + 1) * LANES]
    b_v[...] = wide_v[...].astype(BF16)

    spread(b_v, br_v, bs_sem, br_sem)
    load(br_v.at[rest], br_v.at[rest], br_sem).wait()
    wide_v[...] = br_v[...].astype(F32)
    for q in range(steps):
        for s in range(2):
            s_v[col, s * rows : (s + 1) * rows, q * LANES : (q + 1) * LANES] = wide_v[
                pl.ds(2 * q + s, rows, stride=tile), :
            ].astype(BF16)

    chips = cols // 2
    half = chips // 2
    part = width // PIECES

    def slot(who, q):
        return s_v.at[who, pl.ds(q * part, part)]

    def ring(d, t, q):
        who = lax.rem(col + (cols - 2 * (t - 1) if d == 0 else 2 * (t - 1)), cols)
        return send(slot(who, q), slot(who, q), gs_sem.at[d, t - 1, q], gr_sem.at[d, t - 1, q], (row, right if d == 0 else left))

    def relay(d, t, q):
        who = lax.rem(col + (cols - 2 * t if d == 0 else 2 * t), cols)
        return send(slot(who, q), slot(who, q), cs_sem.at[d, t, q], cr_sem.at[d, t, q], (row, other))

    def uses(d, t):
        if t < half:
            return range(PIECES)
        return range(PIECES // 2) if d == 0 else range(PIECES // 2, PIECES)

    sent = []
    for q in range(PIECES):
        for d in range(2):
            sent.append(ring(d, 1, q))
            sent[-1].start()
    for q in range(PIECES):
        sent.append(relay(0, 0, q))
        sent[-1].start()

    def add(which):
        s = s_v[pl.ds(2 * which, 2)].reshape(2 * width, length)
        acc_v[...] += nn(wt_v[which], s)

    acc_v[...] = jnp.zeros_like(acc_v)
    for q in range(PIECES):
        relay(0, 0, q).wait_recv()
    add(chip)
    for t in range(1, half + 1):
        for q in range(PIECES):
            for d in range(2):
                if q in uses(d, t):
                    ring(d, t, q).wait_recv()
                    if t < half and q in uses(d, t + 1):
                        sent.append(ring(d, t + 1, q))
                        sent[-1].start()
                    sent.append(relay(d, t, q))
                    sent[-1].start()
        for d in range(2):
            for q in uses(d, t):
                relay(d, t, q).wait_recv()
        if t < half:
            add(lax.rem(chip + chips - t, chips))
        add(lax.rem(chip + t, chips))
    for i in range(length // LANES):
        out[i * LANES : (i + 1) * LANES, :] = jnp.transpose(acc_v[:, i * LANES : (i + 1) * LANES]).astype(BF16)

    for c in to_other + to_twin + onward + sent:
        c.wait_send()
    load(a_v.at[rest], a_v.at[rest], as_sem).wait()
    load(b_v.at[rest], b_v.at[rest], bs_sem).wait()


def local(rows, cols, tokens, norm_gain, w_in, w_out):
    length, features = tokens.shape
    width, mapped = w_in.shape[1], w_out.shape[1]
    mix, back, outer, twist, inner, eye = tables(rows, width, length)
    high = rows * length // LANES
    half = cols // 4
    any_spec = pl.BlockSpec(memory_space=pl.ANY)
    dma = pltpu.SemaphoreType.DMA
    return pl.pallas_call(
        functools.partial(kernel, rows, cols),
        out_shape=jax.ShapeDtypeStruct((length, mapped), BF16),
        in_specs=[any_spec] * 10,
        out_specs=pl.BlockSpec(memory_space=pltpu.VMEM),
        scratch_shapes=[
            pltpu.VMEM((length, features), BF16),
            pltpu.VMEM((length // PIECES, features), BF16),
            pltpu.VMEM((length // PIECES, LANES), F32),
            pltpu.VMEM((1, features), F32),
            pltpu.VMEM((features, width), BF16),
            pltpu.VMEM(w_out.shape, BF16),
            pltpu.VMEM(mix.shape, BF16),
            pltpu.VMEM(back.shape, BF16),
            pltpu.VMEM(outer.shape, BF16),
            pltpu.VMEM(twist.shape, F32),
            pltpu.VMEM(inner.shape, BF16),
            pltpu.VMEM(eye.shape, BF16),
            pltpu.VMEM((PIECES, GROUP, length // PIECES), BF16),
            pltpu.VMEM((2 * high, LANES), F32),
            pltpu.VMEM((2 * high, LANES), BF16),
            pltpu.VMEM((2 * high, LANES), BF16),
            pltpu.VMEM((2 * high, LANES), BF16),
            pltpu.VMEM((2 * high, LANES), BF16),
            pltpu.VMEM((cols, width, length), BF16),
            pltpu.VMEM((cols // 2, mapped, 2 * width), BF16),
            pltpu.VMEM((mapped, length), F32),
            dma((PIECES,)),
            dma((9,)),
            dma((3, PIECES)),
            dma((3, PIECES)),
            dma,
            dma,
            dma,
            dma,
            dma((2, half, PIECES)),
            dma((2, half, PIECES)),
            dma((2, half + 1, PIECES)),
            dma((2, half + 1, PIECES)),
        ],
        compiler_params=pltpu.CompilerParams(
            collective_id=0, has_side_effects=True, vmem_limit_bytes=60 * 1024 * 1024
        ),
    )(tokens, norm_gain.reshape(1, features), w_in, w_out, mix, back, outer, twist, inner, eye)


def solution(mesh):
    placed = (P("row", None), P(), P(None, "col"), P(None, "col"))
    return jax.shard_map(
        functools.partial(local, mesh.shape["row"], mesh.shape["col"]),
        mesh=mesh,
        in_specs=placed,
        out_specs=P("row", "col"),
        check_vma=False,
    )
```

```python
import functools
import math

import jax
import jax.numpy as jnp
import ml_dtypes
import numpy as np
from jax import lax
from jax.experimental import pallas as pl
from jax.experimental.pallas import tpu as pltpu
from jax.sharding import PartitionSpec as P

GROUP = 256
NORM_EPS = 1e-06
LANES = 128
X_SIDE = 4
Z_SIDE = 8
PIECES = 4
HALVES = 2
SETS = 4
MESH = pl.DeviceIdType.MESH
FARTHEST_FIRST = sorted(
    [(dz, dx) for dz in range(Z_SIDE) for dx in range(X_SIDE) if dz or dx],
    key=lambda o: (-min(o[0], Z_SIDE - o[0]) - min(o[1], X_SIDE - o[1]), o),
)
BF16 = jnp.bfloat16
F32 = jnp.float32

NEAREST_FIRST = FARTHEST_FIRST[::-1]


def angle(first, second, period):
    return (np.multiply.outer(first, second) % period) * (2.0 * math.pi / period)


def tables(rows, width, length):
    subs = GROUP // width
    pairs = np.arange(GROUP // 2)
    channel = np.arange(GROUP)
    cosine, sine = np.cos(angle(pairs, channel, GROUP)), np.sin(angle(pairs, channel, GROUP))
    sine[0] = np.cos(math.pi * channel)
    mix = np.stack([cosine, sine], 1).reshape(GROUP, GROUP) / math.sqrt(GROUP)

    back = np.zeros((subs, 2, rows, GROUP))
    for p in range(GROUP // 2):
        j, r = divmod(p, rows)
        if p == 0:
            back[j, 0, r, 0] = 1.0
            back[j, 1, r, GROUP // 2] = 1.0
        else:
            back[j, 0, r, p] = back[j, 0, r, GROUP - p] = 1.0
            back[j, 1, r, GROUP - p] = 1.0
            back[j, 1, r, p] = -1.0
    back = back.reshape(subs, 2, SETS, rows // SETS, GROUP).transpose(0, 2, 1, 3, 4).reshape(GROUP, GROUP)

    total = rows * length
    high = total // LANES
    steps = length // LANES
    a = np.arange(high)
    turn = angle(a, a, high)
    outer = np.zeros((2, 2, high, rows, 2, steps))
    for s in range(2):
        outer[s, 0, :, :, s, :] = np.cos(turn).reshape(high, rows, steps)
        outer[s, 1, :, :, s, :] = -np.sin(turn).reshape(high, rows, steps)
    outer = outer.reshape(4 * high, 2 * high) / math.sqrt(high)

    b = np.arange(LANES)
    twist = angle(a, b, total)
    twist = np.concatenate([np.cos(twist), np.sin(twist)], 0)

    turn = angle(b, b, LANES)
    cosine, sine = np.cos(turn), np.sin(turn)
    inner = np.stack([np.concatenate([cosine, sine], 1), np.concatenate([sine, -cosine], 1)]) / math.sqrt(LANES)
    short = ml_dtypes.bfloat16
    return mix.astype(short), back.astype(short), outer.astype(short), twist.astype(np.float32), inner.astype(short), np.eye(width).astype(short)


def nt(a, b):
    return lax.dot_general(a, b, (((1,), (1,)), ((), ())), preferred_element_type=F32)


def nn(a, b):
    return jnp.dot(a, b, preferred_element_type=F32)


def kernel(
    rows, cols,
    tokens, gain, w_in, w_out, mix, back, outer, twist, inner, eye, out,
    tok_v, wg_v, gain_v, win_v, wout_v, mix_v, back_v, outer_v, twist_v, inner_v, eye_v,
    x_v, wide_v, a_v, ar_v, b_v, br_v, s_v, wt_v, acc_v, out_v,
    tok_sem, tab_sem, near_sem, xs_sem, xr_sem, as_sem, ar_sem, bs_sem, br_sem, gs_sem, gr_sem, cs_sem, cr_sem,
):
    length, features = tokens.shape
    width = w_in.shape[0]
    subs = GROUP // width
    piece = length // PIECES
    steps = length // LANES
    tile = 2 * steps
    row, col = lax.axis_index("row"), lax.axis_index("col")
    core = lax.rem(col, 2)
    other = col + 1 - 2 * core
    chip = lax.div(col, 2)
    twin = col + 2 - 4 * lax.rem(chip, 2)
    right, left = lax.rem(col + 2, cols), lax.rem(col + cols - 2, cols)
    j = lax.rem(col, subs)

    def load(src, dst, sem):
        return pltpu.make_async_copy(src, dst, sem)

    def send(src, dst, send_sem, recv_sem, device):
        return pltpu.make_async_remote_copy(
            src_ref=src, dst_ref=dst, send_sem=send_sem, recv_sem=recv_sem, device_id=device, device_id_type=MESH
        )

    z, x = lax.div(row, X_SIDE), lax.rem(row, X_SIDE)
    beside = [(lax.rem(z + Z_SIDE + o, Z_SIDE) * X_SIDE + x, col) for o in (1, -1, 2, -2)]
    near = beside + [(row, other), (row, right), (row, left)]
    near += [(z * X_SIDE + lax.rem(x + i, X_SIDE), col) for i in range(1, X_SIDE)]
    barrier = pltpu.get_barrier_semaphore()
    for mate in near:
        pl.semaphore_signal(barrier, inc=1, device_id=mate, device_id_type=MESH)

    def tell(i):
        for k, mate in enumerate(beside):
            pl.semaphore_signal(near_sem.at[i, k], inc=1, device_id=mate, device_id_type=MESH)

    def hear(i):
        for k in range(len(beside)):
            pl.semaphore_wait(near_sem.at[i, k], 1)

    loads = [load(gain, gain_v, tab_sem.at[0]), load(w_in, win_v, tab_sem.at[1]), load(eye, eye_v, tab_sem.at[2])]
    for c in loads:
        c.start()
    tok = [
        load(tokens.at[pl.ds(p * piece, piece)], tok_v.at[pl.ds(p * piece, piece)], tok_sem.at[p]) for p in range(PIECES)
    ]
    for c in tok:
        c.start()
    later = [
        load(src, dst, tab_sem.at[3 + i])
        for i, (src, dst) in enumerate(
            ((mix, mix_v), (outer, outer_v), (w_out, wout_v), (back, back_v), (twist, twist_v), (inner, inner_v))
        )
    ]
    for c in later:
        c.start()
    with jax.named_scope("wload"):
        for c in loads:
            c.wait()
        wg_v[...] = (win_v[...].astype(F32) * gain_v[...]).astype(BF16)

    def x_slot(p, who):
        return x_v.at[p, pl.ds(pl.multiple_of(lax.rem(who, subs) * width, width), width)]

    to_other = [send(x_slot(p, col), x_slot(p, col), xs_sem, xr_sem.at[0, p], (row, other)) for p in range(PIECES)]
    to_twin = [send(x_slot(p, col), x_slot(p, col), xs_sem, xr_sem.at[1, p], (row, twin)) for p in range(PIECES)]
    onward = [send(x_slot(p, twin), x_slot(p, twin), xs_sem, xr_sem.at[0, p], (row, other)) for p in range(PIECES)]
    block = 64
    for p in range(PIECES):
        with jax.named_scope(f"tokwait{p}"):
            tok[p].wait()
        with jax.named_scope(f"proj{p}"):
            y = nt(tok_v[p * piece : (p + 1) * piece, :], wg_v[...])
            squares = []
            for b in range(piece // block):
                total = jnp.zeros((block, LANES), F32)
                for f in range(0, features, LANES):
                    t = tok_v[pl.ds(p * piece + b * block, block), f : f + LANES].astype(F32)
                    total = total + t * t
                squares.append(jnp.sum(total, axis=1, keepdims=True))
            y = y * lax.rsqrt(jnp.concatenate(squares, 0) * (1.0 / features) + NORM_EPS)
            x_v[p, pl.ds(pl.multiple_of(j * width, width), width), :] = nt(eye_v[...], y.astype(BF16)).astype(BF16)
        if p == 0:
            with jax.named_scope("near"):
                pl.semaphore_wait(barrier, len(near))
            tell(0)
        to_twin[p].start()
        to_other[p].start()
    with jax.named_scope("hear0"):
        hear(0)
        tell(1)

    for c in later:
        c.wait()
    mine = mix_v[pl.ds(pl.multiple_of(j * width, width), width), :]
    for p in range(PIECES + 1):
        if p < PIECES:
            with jax.named_scope(f"twin{p}"):
                to_twin[p].wait_recv()
                onward[p].start()
        if p > 0:
            with jax.named_scope(f"group{p - 1}"):
                both = x_v.at[p - 1, pl.ds(0, 2 * width)]
                load(both, both, xr_sem.at[0, p - 1]).wait()
            with jax.named_scope(f"chan{p - 1}"):
                y = nn(mine, x_v[p - 1])
                for t in range(piece // LANES):
                    wide_v[pl.ds((p - 1) * (piece // LANES) + t, width, stride=steps), :] = y[:, t * LANES : (t + 1) * LANES]
    with jax.named_scope("hear1"):
        hear(1)
    a_v[...] = wide_v[...].astype(BF16)

    def spread(order, src_v, dst_v, send_sem, recv_sem):
        own = pl.ds(pl.multiple_of(row * tile, tile), tile)
        for dz, dx in order:
            d = lax.rem(z + dz, Z_SIDE) * X_SIDE + lax.rem(x + dx, X_SIDE)
            send(
                src_v.at[pl.ds(pl.multiple_of(d * tile, tile), tile)], dst_v.at[own], send_sem, recv_sem, (d, col)
            ).start()
        dst_v[own, :] = src_v[own, :]

    rest = pl.ds(0, (rows - 1) * tile)
    with jax.named_scope("spread1"):
        spread(FARTHEST_FIRST, a_v, ar_v, as_sem, ar_sem)

    per_group = GROUP // (2 * width)
    for g in range(cols // subs):
        wp = nn(back_v[...], wout_v[pl.ds(g * GROUP, GROUP), :])
        for i in range(per_group):
            wt_v[g * per_group + i] = jnp.transpose(wp[i * 2 * width : (i + 1) * 2 * width]).astype(BF16)

    with jax.named_scope("wait1"):
        load(ar_v.at[rest], ar_v.at[rest], ar_sem).wait()

    first = nn(outer_v[...], ar_v[...])
    high = rows * steps
    twist_cos, twist_sin = twist_v[:high], twist_v[high:]
    special = lax.min(j * rows + row, 1)
    for s in range(2):
        re = first[2 * s * high : (2 * s + 1) * high]
        im = first[(2 * s + 1) * high : (2 * s + 2) * high]
        turned = jnp.concatenate([re * twist_cos + im * twist_sin, im * twist_cos - re * twist_sin], axis=1).astype(BF16)
        u = nt(inner_v[0] if s == 0 else inner_v[special], turned)
        for t in range(2):
            wide_v[pl.ds(2 * t + s, LANES, stride=4), :] = u[:, t * LANES : (t + 1) * LANES]
    b_v[...] = wide_v[...].astype(BF16)

    with jax.named_scope("spread2"):
        spread(NEAREST_FIRST, b_v, br_v, bs_sem, br_sem.at[lax.div(z, 2)])
    chips = cols // 2
    half = chips // 2
    part = width // SETS
    lone = rows // SETS
    turn = lax.rem(z, 2)
    first_set = lax.div(z, 2)
    sets = [first_set] + [lax.rem(first_set + o, SETS) for o in (3 - 2 * turn, 1 + 2 * turn, 2)]

    def slot(who, q):
        of_set = pl.ds(pl.multiple_of(sets[q // HALVES] * part, part), part)
        return s_v.at[who, of_set, pl.ds(q % HALVES * (length // HALVES), length // HALVES)]

    def ring(d, t, q):
        who = lax.rem(col + (cols - 2 * (t - 1) if d == 0 else 2 * (t - 1)), cols)
        return send(slot(who, q), slot(who, q), gs_sem, gr_sem.at[d, t - 1, q], (row, right if d == 0 else left))

    def relay(d, t, q):
        who = lax.rem(col + (cols - 2 * t if d == 0 else 2 * t), cols)
        return send(slot(who, q), slot(who, q), cs_sem, cr_sem.at[t], (row, other))

    def uses(d, t):
        if t < half:
            return range(SETS * HALVES)
        return range(d, SETS * HALVES, 2)

    def share(q):
        for c in (ring(0, 1, q), ring(1, 1, q), relay(0, 0, q)):
            c.start()

    for q in range(SETS):
        with jax.named_scope(f"set{q}"):
            came = pl.ds(0, (lone if q else lone - 1) * tile)
            load(br_v.at[came], br_v.at[came], br_sem.at[sets[q]]).wait()
        base = pl.multiple_of(sets[q] * lone * tile, lone * tile)
        wide_v[pl.ds(base, lone * tile), :] = br_v[pl.ds(base, lone * tile), :].astype(F32)
        for k in range(steps):
            if k and k % (steps // HALVES) == 0:
                share(q * HALVES + k // (steps // HALVES) - 1)
            both = [wide_v[pl.ds(base + 2 * k + s, lone, stride=tile), :] for s in range(2)]
            s_v[col, pl.ds(pl.multiple_of(sets[q] * part, part), part), k * LANES : (k + 1) * LANES] = jnp.concatenate(
                both, 0
            ).astype(BF16)
        share(q * HALVES + HALVES - 1)

    def arrived(count, sem):
        blocks = s_v.at[pl.ds(0, count)]
        load(blocks, blocks, sem).wait()

    def add(which):
        acc_v[...] += nn(wt_v[which], s_v[pl.ds(2 * which, 2)].reshape(2 * width, length))

    def gather(t, step):
        if step == 0:
            with jax.named_scope(f"relayed{t}"):
                arrived(1 if t in (0, half) else 2, cr_sem.at[t])
            if t == 0:
                acc_v[...] = nn(wt_v[chip], s_v[pl.ds(2 * chip, 2)].reshape(2 * width, length))
        elif step == 1 and t:
            with jax.named_scope(f"add{t}"):
                add(lax.rem(chip + t, chips))
        elif step == 2 and 0 < t < half:
            with jax.named_scope(f"more{t}"):
                add(lax.rem(chip + chips - t, chips))

    for t in range(1, half + 1):
        for q in range(SETS * HALVES):
            for d in range(2):
                if q in uses(d, t):
                    with jax.named_scope(f"ring{t}q{q}d{d}"):
                        ring(d, t, q).wait_recv()
                    if t < half and q in uses(d, t + 1):
                        ring(d, t + 1, q).start()
                    relay(d, t, q).start()
            if q % 2 and q > 1:
                gather(t - 1, q // 2 - 1)
    for step in range(2):
        gather(half, step)
    with jax.named_scope("final"):
        for i in range(length // LANES):
            out_v[i * LANES : (i + 1) * LANES, :] = jnp.transpose(acc_v[:, i * LANES : (i + 1) * LANES]).astype(BF16)
    store = load(out_v, out, tab_sem.at[0])
    store.start()

    exchanged = x_v.at[pl.ds(0, 3 * PIECES * width // GROUP)]
    load(exchanged, exchanged, xs_sem).wait()
    arrived(cols // 2 - 1, gs_sem)
    arrived(cols // 2, cs_sem)
    load(a_v.at[rest], a_v.at[rest], as_sem).wait()
    load(b_v.at[rest], b_v.at[rest], bs_sem).wait()
    with jax.named_scope("stored"):
        store.wait()


def local(rows, cols, tokens, norm_gain, w_in, w_out):
    length, features = tokens.shape
    width, mapped = w_in.shape[1], w_out.shape[1]
    mix, back, outer, twist, inner, eye = tables(rows, width, length)
    high = rows * length // LANES
    half = cols // 4
    any_spec = pl.BlockSpec(memory_space=pl.ANY)
    dma = pltpu.SemaphoreType.DMA
    return pl.pallas_call(
        functools.partial(kernel, rows, cols),
        out_shape=jax.ShapeDtypeStruct((length, mapped), BF16),
        in_specs=[any_spec] * 10,
        out_specs=any_spec,
        scratch_shapes=[
            pltpu.VMEM((length, features), BF16),
            pltpu.VMEM((width, features), BF16),
            pltpu.VMEM((1, features), F32),
            pltpu.VMEM((width, features), BF16),
            pltpu.VMEM(w_out.shape, BF16),
            pltpu.VMEM(mix.shape, BF16),
            pltpu.VMEM(back.shape, BF16),
            pltpu.VMEM(outer.shape, BF16),
            pltpu.VMEM(twist.shape, F32),
            pltpu.VMEM(inner.shape, BF16),
            pltpu.VMEM(eye.shape, BF16),
            pltpu.VMEM((PIECES, GROUP, length // PIECES), BF16),
            pltpu.VMEM((2 * high, LANES), F32),
            pltpu.VMEM((2 * high, LANES), BF16),
            pltpu.VMEM((2 * high, LANES), BF16),
            pltpu.VMEM((2 * high, LANES), BF16),
            pltpu.VMEM((2 * high, LANES), BF16),
            pltpu.VMEM((cols, width, length), BF16),
            pltpu.VMEM((cols // 2, mapped, 2 * width), BF16),
            pltpu.VMEM((mapped, length), F32),
            pltpu.VMEM((length, mapped), BF16),
            dma((PIECES,)),
            dma((9,)),
            pltpu.SemaphoreType.REGULAR((2, 4)),
            dma,
            dma((2, PIECES)),
            dma,
            dma,
            dma,
            dma((SETS,)),
            dma,
            dma((2, half, SETS * HALVES)),
            dma,
            dma((half + 1,)),
        ],
        compiler_params=pltpu.CompilerParams(
            collective_id=0, has_side_effects=True, vmem_limit_bytes=60 * 1024 * 1024
        ),
    )(tokens, norm_gain.reshape(1, features), w_in.T, w_out, mix, back, outer, twist, inner, eye)


def solution(mesh):
    placed = (P("row", None), P(), P(None, "col"), P(None, "col"))
    return jax.shard_map(
        functools.partial(local, mesh.shape["row"], mesh.shape["col"]),
        mesh=mesh,
        in_specs=placed,
        out_specs=P("row", "col"),
        check_vma=False,
    )
```
